32 devices in a mesh: sp: 8 (over z, x), tp: 4 (over y, core).
Axes of the slice: x: 2, y: 2, z: 4, core: 2. Of those that a mesh axis runs over, the one named last changes fastest.
Arguments:
- outer_gate: bfloat16 [2048, 2048], P('sp', 'tp'), may hold values from -6 to 6
- inner_gate: bfloat16 [2048, 2048], P('sp', 'tp'), may hold values from -6 to 6
- conv_input: bfloat16 [2048, 2048], P('sp', 'tp'), may hold values from -6 to 6
- conv_weight: bfloat16 [3, 2048], P(None, 'tp'), may hold values from -3.5 to 3.5
- doc_ids: int32 [2048], P('sp'), may hold values from 0 to 3, as said below
- output_weight: bfloat16 [2048, 4096], P(None, 'tp'), may hold values from -0.125 to 0.125
- residual: bfloat16 [2048, 4096], P('sp', 'tp'), as said below
- norm_gain: bfloat16 [4096], P('tp'), may hold values from 0.099609375 to 1.8984375
- expert_ids: int32 [2048, 2], P('sp'), may hold values from 0 to 7, all different within a row; in each aligned block of 256 rows (0 to 255, 256 to 511, ...) at most 128 rows name the same one
- group_weight: float32 [2048], P('sp'), may hold values from 0.25 to 1
- expert_weight: float32 [2048, 2], P('sp'), may hold values from 0.05 to 1
- gate_weight: bfloat16 [8, 4096, 2048], P('sp', None, 'tp'), may hold values from -0.09375 to 0.09375
- up_weight: bfloat16 [8, 4096, 2048], P('sp', None, 'tp'), may hold values from -0.09375 to 0.09375
- down_weight: bfloat16 [8, 2048, 4096], P('sp', None, 'tp'), may hold values from -0.125 to 0.125
Outputs:
- layer_out: bfloat16 [2048, 4096], P('sp', 'tp')
The draws below stay inside these ranges and needn't reach their ends.
Inputs may be any that keep to these rules, and one draw needn't show every extreme that they name: `expert_ids`: within the 256 rows of one index of sp no expert is named more than 128 times, a bound that some block reaches; the two experts of a row differ. `doc_ids`: never falling along positions, rising by one at each document's start; every document has 256 to 768 positions, and one exactly 768. `residual`: Columns' scales are of order one to ten.
All inputs are finite; a program needn't handle non-finite values.
Results may differ from the reference program's by a relative error of at most 0.009.
Values may be sent and summed in bfloat16 or wider, within the bound.
A program may use at most 64 MiB of HBM per device.

```python
import math
import jax
import jax.numpy as jnp
import numpy as np
from jax import lax

D = 4096
BRANCH = 2048
FFN = 2048
TAPS = 3
TOK = 256
TOKENS = 2048
EXPERTS = 8
CAP = 128
N_SP = 8


def draw_residual(key, part):
    column_scale = 10.0 ** (jnp.arange(D, dtype=jnp.float32) / D)
    base = jax.random.normal(key, (TOKENS, D), jnp.float32)
    return (base * column_scale * 0.5).astype(jnp.bfloat16)


def draw_doc_ids(key, part):
    bound_total = N_SP // 2 - 1
    jitters = jax.random.randint(jax.random.fold_in(key, 11), (bound_total,), 0, TOK, dtype=jnp.int32)
    longest = jax.random.randint(jax.random.fold_in(key, 13), (), 0, bound_total, dtype=jnp.int32)
    marker = jnp.arange(bound_total, dtype=jnp.int32)
    jitters = jnp.where(marker == longest - 1, 0, jitters)
    jitters = jnp.where(marker == longest, TOK, jitters)
    starts = (marker + 1) * (2 * TOK) + jitters
    positions = jnp.arange(TOKENS, dtype=jnp.int32)
    return jnp.sum((positions[:, None] >= starts[None, :]).astype(jnp.int32), axis=1).astype(jnp.int32)


def level_of(rng, extent, pieces, least, largest):
    loudness, own = 1.0, jax.random.fold_in(rng, 6)
    for axis_at, blocks in pieces:
        heights = jnp.exp(jax.random.uniform(jax.random.fold_in(own, axis_at), (blocks,), jnp.float32, least / len(pieces), largest / len(pieces)))
        loudness = loudness * jnp.repeat(heights, extent[axis_at] // blocks).reshape([-1 if axis == axis_at else 1 for axis in range(len(extent))])
    return loudness


def deal_out(stream_key, own, number, rows, amount, top, bound, lean):
    sequence = jax.random.permutation(stream_key, amount)
    heavy_load, ordinary = shares(amount, rows * top, bound, lean, True), shares(amount, rows * top, bound, lean, False)
    places = jnp.arange(amount)

    def named(tallies, turn):
        used = int((tallies > 0).sum())
        fixed = max(1, used // 4)
        moved = fixed + (places - fixed + turn * (used - fixed)) % max(1, amount - fixed)
        return jnp.zeros((amount,), jnp.int32).at[sequence[jnp.where(places < fixed, places, moved)]].set(jnp.asarray(tallies, jnp.int32))

    tallies = jnp.where(number % 4 == 0, named(heavy_load, number // 4), named(ordinary, number - number // 4 - 1))
    mixed = jax.random.permutation(jax.random.fold_in(own, 3), amount)
    source_of, sink = mixed[0:amount // 2 * 2:2], mixed[1:amount // 2 * 2:2]
    margin = jnp.minimum(tallies[source_of] - 1, bound - tallies[sink]) // 2
    margin = jnp.where((source_of == sequence[0]) | (sink == sequence[0]) | (tallies[sink] == 0), 0, jnp.maximum(margin, 0))
    moved = jax.random.randint(jax.random.fold_in(own, 4), (amount // 2,), 0, 1 << 20) % (margin + 1)
    tallies = tallies.at[source_of].add(-moved).at[sink].add(moved)
    items = jnp.searchsorted(jnp.cumsum(tallies), jnp.arange(rows * top), side="right").astype(jnp.int32)
    grid = items.reshape(top, rows).T
    grid = grid[jax.random.permutation(jax.random.fold_in(own, 1), rows)]
    turn = jax.random.randint(jax.random.fold_in(own, 2), (rows, 1), 0, top)
    return jnp.take_along_axis(grid, (jnp.arange(top)[None, :] + turn) % top, axis=1)


def shares(count, total, reach, skew, full):
    portions = [(1 << 20) // math.isqrt(rank ** skew) + 1 for rank in range(1, count + 1)]
    largest = reach if full else min(reach, max(-(-total // count), total * portions[0] // sum(portions)))
    least = 1 if total - largest >= count - 1 else 0
    counts, rest = [largest] + [least] * (count - 1), total - largest - least * (count - 1)
    while rest > 0:
        candidates = [i for i in range(1, count) if counts[i] < largest] or [i for i in range(1, count) if counts[i] < reach]
        whole, remaining = sum([portions[i] for i in candidates]), rest
        for i in candidates:
            more = min(reach - counts[i], max(1, remaining * portions[i] // whole), rest)
            counts[i] = counts[i] + more
            rest = rest - more
    return np.array(counts)


def centred(rng, extent, width, limit, cuts=(), kind=jnp.bfloat16):
    values = jax.random.normal(rng, extent, jnp.float32) * width
    if len(cuts) > 0:
        values = level_of(rng, extent, cuts, -0.22, 0.18) * values
    return jnp.clip(values, min=-limit, max=limit).astype(kind)


def setup_inputs(seed: int = 0) -> dict:
    key_of = jax.random.split(jax.random.key(seed), 15)
    outer_gate = centred(key_of[0], (TOKENS, BRANCH), 1.0, 6.0, ((0, 8), (1, 4)))
    inner_gate = centred(key_of[1], (TOKENS, BRANCH), 1.0, 6.0, ((0, 8), (1, 4)))
    conv_input = centred(key_of[2], (TOKENS, BRANCH), 1.0, 6.0, ((0, 8), (1, 4)))
    conv_weight = centred(key_of[3], (TAPS, BRANCH), TAPS ** -0.5, 3.5, ((1, 4),))
    doc_ids = draw_doc_ids(jax.random.fold_in(key_of[14], 71), 0)
    output_weight = centred(key_of[5], (BRANCH, D), BRANCH ** -0.5, 0.125, ((1, 4),))
    residual = draw_residual(jax.random.fold_in(key_of[14], 71), 0)
    norm_gain = jnp.clip(1.0 + 0.18 * jax.random.normal(key_of[7], (D,), jnp.float32), 0.099609375, 1.8984375).astype(jnp.bfloat16)
    expert_ids_keys = jax.random.split(jax.random.fold_in(key_of[8], 1), TOKENS // TOK)
    expert_ids_turns = jax.random.permutation(jax.random.fold_in(key_of[8], 3), TOKENS // TOK)
    expert_ids = jax.vmap(lambda own, number: deal_out(jax.random.fold_in(key_of[8], 2), own, number, TOK, EXPERTS, 2, CAP, 2))(expert_ids_keys, expert_ids_turns).reshape((TOKENS, 2))
    group_weight = jnp.clip(0.25 + 0.75 * jax.random.uniform(key_of[9], (TOKENS,), jnp.float32) ** level_of(key_of[9], (TOKENS,), ((0, 8),), -0.2, 0.2), 0.25, 1.0)
    expert_weight = jnp.clip(jnp.exp(math.log(1.0) - 2.9957323 * jax.random.uniform(key_of[10], (TOKENS, 2), jnp.float32) ** level_of(key_of[10], (TOKENS, 2), ((0, 8),), -0.2, 0.2)), 0.05, 1.0)
    gate_weight = centred(key_of[11], (EXPERTS, D, FFN), D ** -0.5, 0.09375, ((0, 8), (2, 4)))
    up_weight = centred(key_of[12], (EXPERTS, D, FFN), D ** -0.5, 0.09375, ((0, 8), (2, 4)))
    down_weight = centred(key_of[13], (EXPERTS, FFN, D), FFN ** -0.5, 0.125, ((0, 8), (2, 4)))
    return {"outer_gate": outer_gate, "inner_gate": inner_gate, "conv_input": conv_input, "conv_weight": conv_weight, "doc_ids": doc_ids, "output_weight": output_weight, "residual": residual, "norm_gain": norm_gain, "expert_ids": expert_ids, "group_weight": group_weight, "expert_weight": expert_weight, "gate_weight": gate_weight, "up_weight": up_weight, "down_weight": down_weight}


EPS = 1e-06

def reference(outer_gate, inner_gate, conv_input, conv_weight, doc_ids, output_weight, residual, norm_gain, expert_ids, group_weight, expert_weight, gate_weight, up_weight, down_weight):
    products = inner_gate.astype(jnp.float32) * conv_input.astype(jnp.float32)
    taps = conv_weight.astype(jnp.float32)
    conv = taps[2] * products
    for shift_by in (1, 2):
        earlier = jnp.pad(products, ((shift_by, 0), (0, 0)))[:-shift_by]
        earlier_docs = jnp.pad(doc_ids, (shift_by, 0), constant_values=-1)[:-shift_by]
        same_doc = (earlier_docs == doc_ids)[:, None]
        conv = conv + jnp.where(same_doc, taps[2 - shift_by] * earlier, 0.0)
    branch = (outer_gate.astype(jnp.float32) * conv).astype(jnp.bfloat16)
    branch_sum = jnp.dot(branch, output_weight, preferred_element_type=jnp.float32)
    resid = (residual.astype(jnp.float32) + branch_sum).astype(jnp.bfloat16)
    resid_wide = resid.astype(jnp.float32)
    scale = lax.rsqrt(lax.optimization_barrier(jnp.mean(resid_wide * resid_wide, axis=1, keepdims=True)) + EPS)
    normed = (resid_wide * scale * norm_gain.astype(jnp.float32)).astype(jnp.bfloat16)
    mix_weight = group_weight[:, None] * expert_weight / lax.optimization_barrier(jnp.sum(expert_weight, axis=1, keepdims=True))
    flat_experts = expert_ids.reshape(N_SP, 2 * TOK)
    onehot = (flat_experts[:, :, None] == jnp.arange(EXPERTS, dtype=jnp.int32)[None, None, :]).astype(jnp.int32)
    slot_rank = lax.optimization_barrier(jnp.sum((jnp.cumsum(onehot, axis=1) - onehot) * onehot, axis=2)).astype(jnp.int32)
    slot_index = flat_experts * CAP + slot_rank
    token_of = jnp.broadcast_to(jnp.arange(2 * TOK, dtype=jnp.int32) // 2, slot_index.shape)
    group_index = jnp.arange(N_SP, dtype=jnp.int32)[:, None]
    token_table = jnp.full((N_SP, EXPERTS * CAP), TOK, jnp.int32).at[group_index, slot_index].set(token_of)
    token_table = token_table.reshape(N_SP, EXPERTS, CAP)
    grouped = jnp.concatenate([normed.reshape(N_SP, TOK, D), jnp.zeros((N_SP, 1, D), jnp.bfloat16)], axis=1)

    def one_expert(expert):
        chosen = lax.dynamic_index_in_dim(token_table, expert, 1, keepdims=False)
        routed = grouped[group_index, chosen].reshape(N_SP * CAP, D)
        gate_val = jnp.dot(routed, gate_weight[expert], preferred_element_type=jnp.float32)
        up_val = jnp.dot(routed, up_weight[expert], preferred_element_type=jnp.float32)
        hidden = (jax.nn.silu(gate_val) * up_val).astype(jnp.bfloat16)
        result = jnp.dot(hidden, down_weight[expert], preferred_element_type=jnp.float32).astype(jnp.bfloat16)
        return result.reshape(N_SP, CAP, D)
    expert_out = lax.map(one_expert, jnp.arange(EXPERTS, dtype=jnp.int32))
    picked = expert_out[flat_experts, group_index, slot_rank].reshape(TOKENS, 2, D).astype(jnp.float32)
    routed_sum = lax.optimization_barrier(jnp.sum(picked * mix_weight[:, :, None], axis=1))
    return (resid_wide + routed_sum).astype(jnp.bfloat16)
```

```python
import functools

import jax
import jax.numpy as jnp
from jax import lax
from jax.experimental import pallas as pl
from jax.experimental.pallas import tpu as pltpu
from jax.sharding import PartitionSpec as P

EPS = 1e-06
MESH = pl.DeviceIdType.MESH


def remote(src, dst, send_sem, recv_sem, device):
    return pltpu.make_async_remote_copy(
        src_ref=src,
        dst_ref=dst,
        send_sem=send_sem,
        recv_sem=recv_sem,
        device_id=device,
        device_id_type=MESH,
    )


def expert_kernel(
    n,
    tp,
    out_ref,
    gate_hbm,
    up_hbm,
    down_hbm,
    ret_ref,
    piece,
    hid,
    eo,
    gate_w,
    up_w,
    down_w,
    w_sem,
    own_sem,
    a_send,
    a_recv,
    y_send,
    y_recv,
    p_send,
    p_recv,
    hy_send,
    hy_recv,
    hp_send,
    hp_recv,
    r_send,
    r_recv,
):
    me = lax.axis_index("sp")
    t = lax.axis_index("tp")
    chips = tp // 2
    y, core = lax.div(t, 2), lax.rem(t, 2)
    partner = t + 1 - 2 * core
    cap, cols = out_ref.shape[1], out_ref.shape[2]
    ffn_local = gate_w.shape[1]
    groups, group_rows = hid.shape[0], hid.shape[1]
    fans = p_send.shape[1]
    fan_blocks = n // fans
    group_fans = fans // groups
    group_blocks = n // groups

    def column(index, width):
        return pl.ds(pl.multiple_of(index * width, 128), width)

    def chip_at(delta):
        return lax.rem(y + delta + chips, chips) * 2 + core

    weight_copies = [
        pltpu.make_async_copy(source.at[0], target, w_sem.at[i])
        for i, (source, target) in enumerate(
            ((gate_hbm, gate_w), (up_hbm, up_w), (down_hbm, down_w))
        )
    ]
    for copy in weight_copies:
        copy.start()

    barrier = pltpu.get_barrier_semaphore()
    for k in range(1, n):
        pl.semaphore_signal(
            barrier, inc=1, device_id=(lax.rem(me + k, n), t), device_id_type=MESH
        )
    pl.semaphore_signal(barrier, inc=1, device_id=(me, partner), device_id_type=MESH)
    for d in range(1, chips):
        pl.semaphore_signal(barrier, inc=1, device_id=(me, chip_at(d)), device_id_type=MESH)
    pl.semaphore_wait(barrier, n - 1 + chips)

    own_in = pltpu.make_async_copy(out_ref.at[me], piece.at[0, :, column(t, cols)], own_sem.at[0])
    own_in.start()
    sends = []
    arrivals = []
    for k in range(1, n):
        there = lax.rem(me + k, n)
        copy = remote(
            out_ref.at[there],
            piece.at[k, :, column(t, cols)],
            a_send.at[k],
            a_recv.at[k],
            (there, t),
        )
        copy.start()
        sends.append(copy)
        arrivals.append(copy)

    def fan_region(f, index):
        return piece.at[pl.ds(f * fan_blocks, fan_blocks), :, column(index, cols)]

    def fan_out(f):
        for k in range(f * fan_blocks, (f + 1) * fan_blocks):
            if k == 0:
                own_in.wait()
            else:
                arrivals[k - 1].wait_recv()
        region = fan_region(f, t)
        for d in range(1, chips):
            copy = remote(
                region, region, y_send.at[d, f], y_recv.at[d, f], (me, chip_at(d))
            )
            copy.start()
            sends.append(copy)
        copy = remote(region, region, p_send.at[0, f], p_recv.at[0, f], (me, partner))
        copy.start()
        sends.append(copy)

    def relay(f):
        for d in range(1, chips):
            source = chip_at(-d)
            region = fan_region(f, source)
            remote(
                region, region, y_send.at[d, f], y_recv.at[d, f], (me, partner)
            ).wait_recv()
            copy = remote(region, region, p_send.at[d, f], p_recv.at[d, f], (me, partner))
            copy.start()
            sends.append(copy)

    def hid_region(g, index):
        return hid.at[g, :, column(index, ffn_local)]

    def up_stage(g):
        for f in range(g * group_fans, (g + 1) * group_fans):
            for d in range(chips):
                region = fan_region(f, chip_at(-d) + partner - t)
                remote(
                    region, region, p_send.at[d, f], p_recv.at[d, f], (me, partner)
                ).wait_recv()
        if g == 0:
            weight_copies[0].wait()
            weight_copies[1].wait()
        step = min(256, ffn_local)

        def tile(j, carry):
            rows = piece[pl.ds(g * group_blocks, group_blocks)].reshape(group_rows, tp * cols)
            at = pl.ds(pl.multiple_of(j * step, 128), step)
            gate_val = jnp.dot(rows, gate_w[:, at], preferred_element_type=jnp.float32)
            up_val = jnp.dot(rows, up_w[:, at], preferred_element_type=jnp.float32)
            hidden = (jax.nn.silu(gate_val) * up_val).astype(jnp.bfloat16)
            hid[g, :, pl.ds(pl.multiple_of(t * ffn_local + j * step, 128), step)] = hidden
            return carry

        lax.fori_loop(0, ffn_local // step, tile, 0)
        region = hid_region(g, t)
        for d in range(1, chips):
            copy = remote(
                region, region, hy_send.at[d, g], hy_recv.at[d, g], (me, chip_at(d))
            )
            copy.start()
            sends.append(copy)
        copy = remote(region, region, hp_send.at[0, g], hp_recv.at[0, g], (me, partner))
        copy.start()
        sends.append(copy)

    def relay_hidden(g):
        for d in range(1, chips):
            region = hid_region(g, chip_at(-d))
            remote(
                region, region, hy_send.at[d, g], hy_recv.at[d, g], (me, partner)
            ).wait_recv()
            copy = remote(region, region, hp_send.at[d, g], hp_recv.at[d, g], (me, partner))
            copy.start()
            sends.append(copy)

    returns = []

    def down_stage(g):
        for d in range(chips):
            region = hid_region(g, chip_at(-d) + partner - t)
            remote(
                region, region, hp_send.at[d, g], hp_recv.at[d, g], (me, partner)
            ).wait_recv()
        if g == 0:
            weight_copies[2].wait()
        step = min(256, cols)

        def tile(j, carry):
            at = pl.ds(pl.multiple_of(j * step, 128), step)
            value = jnp.dot(hid[g], down_w[:, at], preferred_element_type=jnp.float32)
            eo[pl.ds(g * group_blocks, group_blocks), :, at] = value.astype(
                jnp.bfloat16
            ).reshape(group_blocks, cap, step)
            return carry

        lax.fori_loop(0, cols // step, tile, 0)
        for k in range(g * group_blocks, (g + 1) * group_blocks):
            if k == 0:
                copy = pltpu.make_async_copy(eo.at[0], ret_ref.at[me], own_sem.at[1])
            else:
                copy = remote(
                    eo.at[k],
                    ret_ref.at[me],
                    r_send.at[k],
                    r_recv.at[k],
                    (lax.rem(me + n - k, n), t),
                )
            copy.start()
            returns.append(copy)

    def fans_of(g):
        return range(g * group_fans, (g + 1) * group_fans)

    ahead = min(2, groups)
    for g in range(ahead):
        for f in fans_of(g):
            fan_out(f)
    for g in range(groups):
        for f in fans_of(g):
            relay(f)
        up_stage(g)
        if g + ahead < groups:
            for f in fans_of(g + ahead):
                fan_out(f)
        if g >= 1:
            relay_hidden(g - 1)
            down_stage(g - 1)
    relay_hidden(groups - 1)
    down_stage(groups - 1)

    for k, copy in enumerate(returns):
        if k == 0:
            copy.wait()
        else:
            there = lax.rem(me + k, n)
            copy.wait_send()
            remote(
                eo.at[k], ret_ref.at[there], r_send.at[k], r_recv.at[k], (there, t)
            ).wait_recv()
    for copy in sends:
        copy.wait_send()


def expert_layer(outgoing, gate_weight, up_weight, down_weight):
    n, tp = lax.axis_size("sp"), lax.axis_size("tp")
    cap, cols = outgoing.shape[1], outgoing.shape[2]
    chips = tp // 2
    rows = n * cap
    groups = max(1, min(4, rows // 256))
    fans = min(n, 2 * groups)
    width, ffn_local = gate_weight.shape[1], gate_weight.shape[2]
    ffn = down_weight.shape[1]
    dma = pltpu.SemaphoreType.DMA
    flops = 2 * rows * width * ffn_local * 2 + 2 * rows * ffn * cols
    return pl.pallas_call(
        functools.partial(expert_kernel, n, tp),
        out_shape=jax.ShapeDtypeStruct(outgoing.shape, jnp.bfloat16),
        in_specs=[pl.BlockSpec(memory_space=pltpu.VMEM)]
        + [pl.BlockSpec(memory_space=pl.ANY)] * 3,
        out_specs=pl.BlockSpec(memory_space=pltpu.VMEM),
        scratch_shapes=[
            pltpu.VMEM((n, cap, width), jnp.bfloat16),
            pltpu.VMEM((groups, rows // groups, ffn), jnp.bfloat16),
            pltpu.VMEM((n, cap, cols), jnp.bfloat16),
            pltpu.VMEM((width, ffn_local), jnp.bfloat16),
            pltpu.VMEM((width, ffn_local), jnp.bfloat16),
            pltpu.VMEM((ffn, cols), jnp.bfloat16),
            dma((3,)),
            dma((2,)),
            dma((n,)),
            dma((n,)),
            dma((chips, fans)),
            dma((chips, fans)),
            dma((chips, fans)),
            dma((chips, fans)),
            dma((chips, groups)),
            dma((chips, groups)),
            dma((chips, groups)),
            dma((chips, groups)),
            dma((n,)),
            dma((n,)),
        ],
        compiler_params=pltpu.CompilerParams(
            collective_id=0, has_side_effects=True, vmem_limit_bytes=48 * 1024 * 1024
        ),
        cost_estimate=pl.CostEstimate(
            flops=flops, bytes_accessed=3 * width * ffn_local * 2, transcendentals=0
        ),
        name="experts",
    )(outgoing, gate_weight, up_weight, down_weight)


def passed_along(value, axis, steps):
    count = lax.axis_size(axis)
    initial, last = (max(0, -steps), min(count, count - steps))
    return lax.ppermute(value, axis, [(source, source + steps) for source in range(initial, last)])


def per_device(
    outer_gate,
    inner_gate,
    conv_input,
    conv_weight,
    doc_ids,
    output_weight,
    residual,
    norm_gain,
    expert_ids,
    group_weight,
    expert_weight,
    gate_weight,
    up_weight,
    down_weight,
):
    row_count = conv_input.shape[0]
    products = inner_gate.astype(jnp.float32) * conv_input.astype(jnp.float32)
    own_docs = doc_ids.astype(jnp.float32)
    tail_rows, tail_docs = passed_along((products[-2:], own_docs[-2:]), "sp", 1)
    ext_products = jnp.concatenate([tail_rows, products], axis=0)
    ext_docs = jnp.concatenate([tail_docs, own_docs], axis=0)
    taps = conv_weight.astype(jnp.float32)
    conv = taps[2] * products
    for shift_by in (1, 2):
        first = 2 - shift_by
        same_doc = (ext_docs[first : first + row_count] == own_docs)[:, None]
        conv = conv + jnp.where(
            same_doc, taps[2 - shift_by] * ext_products[first : first + row_count], 0.0
        )
    branch = (outer_gate.astype(jnp.float32) * conv).astype(jnp.bfloat16)
    cols_local = output_weight.shape[1]
    branch_sum = jnp.dot(
        lax.all_gather(branch, "tp", axis=1, tiled=True),
        output_weight,
        preferred_element_type=jnp.float32,
    )
    resid = (residual.astype(jnp.float32) + branch_sum).astype(jnp.bfloat16)
    resid_wide = resid.astype(jnp.float32)
    total_sq = lax.psum(jnp.sum(resid_wide * resid_wide, axis=1), "tp")
    width = cols_local * lax.axis_size("tp")
    scale = lax.rsqrt(total_sq / width + EPS)[:, None]
    normed = (resid_wide * scale * norm_gain.astype(jnp.float32)).astype(jnp.bfloat16)
    experts = lax.axis_size("sp")
    capacity = 4 * row_count // experts
    flat_experts = expert_ids.reshape(-1)
    onehot = (flat_experts[:, None] == jnp.arange(experts, dtype=jnp.int32)[None, :]).astype(
        jnp.int32
    )
    slot_rank = jnp.sum((jnp.cumsum(onehot, axis=0) - onehot) * onehot, axis=1)
    slot_index = flat_experts * capacity + slot_rank
    slots = slot_index.reshape(row_count, 2)
    arrived_rows = experts * capacity
    slot_iota = jnp.arange(arrived_rows, dtype=jnp.int32)[:, None]
    select = (
        (slot_iota == slots[:, 0][None, :]) | (slot_iota == slots[:, 1][None, :])
    ).astype(jnp.bfloat16)
    outgoing = (
        jnp.dot(select, normed, preferred_element_type=jnp.float32)
        .astype(jnp.bfloat16)
        .reshape(experts, capacity, cols_local)
    )
    returned = expert_layer(outgoing, gate_weight, up_weight, down_weight)
    picked = (
        returned.reshape(arrived_rows, cols_local)[slot_index]
        .reshape(row_count, 2, cols_local)
        .astype(jnp.float32)
    )
    mix_weight = (
        group_weight[:, None] * expert_weight / jnp.sum(expert_weight, axis=1, keepdims=True)
    )
    routed_sum = jnp.sum(picked * mix_weight[:, :, None], axis=1)
    return (resid_wide + routed_sum).astype(jnp.bfloat16)


def solution(mesh):
    return jax.shard_map(
        per_device,
        mesh=mesh,
        in_specs=(
            P("sp", "tp"),
            P("sp", "tp"),
            P("sp", "tp"),
            P(None, "tp"),
            P("sp"),
            P(None, "tp"),
            P("sp", "tp"),
            P("tp"),
            P("sp", None),
            P("sp"),
            P("sp", None),
            P("sp", None, "tp"),
            P("sp", None, "tp"),
            P("sp", None, "tp"),
        ),
        out_specs=P("sp", "tp"),
        check_vma=False,
    )
```

```python
import functools

import jax
import jax.numpy as jnp
from jax import lax
from jax.experimental import pallas as pl
from jax.experimental.pallas import tpu as pltpu
from jax.sharding import PartitionSpec as P

EPS = 1e-06
MESH = pl.DeviceIdType.MESH


def remote(src, dst, send_sem, recv_sem, device):
    return pltpu.make_async_remote_copy(
        src_ref=src,
        dst_ref=dst,
        send_sem=send_sem,
        recv_sem=recv_sem,
        device_id=device,
        device_id_type=MESH,
    )


def expert_kernel(
    n,
    tp,
    outer_ref,
    inner_ref,
    conv_ref,
    taps_ref,
    docs_ref,
    residual_ref,
    gain_ref,
    ids_ref,
    mix_ref,
    proj_hbm,
    gate_hbm,
    up_hbm,
    down_hbm,
    result_ref,
    out_ref,
    ret_ref,
    branch,
    proj_w,
    acc,
    resid,
    normed,
    squares,
    key_col,
    key_row,
    mix_col,
    halo_inner,
    halo_conv,
    halo_docs,
    piece,
    hid,
    eo,
    gate_w,
    up_w,
    down_w,
    w_sem,
    own_sem,
    a_send,
    a_recv,
    y_send,
    y_recv,
    p_send,
    p_recv,
    hy_send,
    hy_recv,
    hp_send,
    hp_recv,
    r_send,
    r_recv,
    h_send,
    h_recv,
    by_send,
    by_recv,
    bp_send,
    bp_recv,
    s_send,
    s_recv,
):
    me = lax.axis_index("sp")
    t = lax.axis_index("tp")
    chips = tp // 2
    y, core = lax.div(t, 2), lax.rem(t, 2)
    partner = t + 1 - 2 * core
    cap, cols = out_ref.shape[1], out_ref.shape[2]
    ffn_local = gate_w.shape[1]
    groups, group_rows = hid.shape[0], hid.shape[1]
    fans = p_send.shape[1]
    fan_blocks = n // fans
    group_fans = fans // groups
    group_blocks = n // groups

    def column(index, width):
        return pl.ds(pl.multiple_of(index * width, 128), width)

    def chip_at(delta):
        return lax.rem(y + delta + chips, chips) * 2 + core

    weight_copies = [
        pltpu.make_async_copy(source, target, w_sem.at[i])
        for i, (source, target) in enumerate(
            (
                (gate_hbm.at[0], gate_w),
                (up_hbm.at[0], up_w),
                (down_hbm.at[0], down_w),
                (proj_hbm, proj_w),
            )
        )
    ]
    for i in (3, 0, 1, 2):
        weight_copies[i].start()

    barrier = pltpu.get_barrier_semaphore()
    for k in range(1, n):
        pl.semaphore_signal(
            barrier, inc=1, device_id=(lax.rem(me + k, n), t), device_id_type=MESH
        )
    for d in range(1, tp):
        pl.semaphore_signal(
            barrier, inc=1, device_id=(me, lax.rem(t + d, tp)), device_id_type=MESH
        )
    pl.semaphore_wait(barrier, n - 1 + tp - 1)

    sends = []
    arrivals = []
    row_count = residual_ref.shape[0]
    wide = branch.shape[1] // tp

    halos = []
    following = (lax.rem(me + 1, n), t)
    for i, (source, target) in enumerate(
        (
            (inner_ref.at[pl.ds(row_count - 16, 16)], halo_inner),
            (conv_ref.at[pl.ds(row_count - 16, 16)], halo_conv),
            (docs_ref.at[pl.ds(row_count - 8, 8)], halo_docs),
        )
    ):
        copy = remote(source, target, h_send.at[i], h_recv.at[i], following)
        copy.start()
        halos.append(copy)
        sends.append(copy)

    lanes = lax.broadcasted_iota(jnp.int32, (row_count, 128), 1)
    first_id, second_id = ids_ref[:, 0:1], ids_ref[:, 1:2]
    is_first, is_second = lanes == first_id, lanes == second_id
    mix_col[...] = jnp.where(is_first, mix_ref[:, 0:1], 0.0) + jnp.where(
        is_second, mix_ref[:, 1:2], 0.0
    )
    member = jnp.where(is_first, 1.0, 0.0) + jnp.where(is_second, 1.0, 0.0)
    earlier = jnp.where(
        lax.broadcasted_iota(jnp.int32, (row_count, row_count), 1)
        < lax.broadcasted_iota(jnp.int32, (row_count, row_count), 0),
        1.0,
        0.0,
    ).astype(jnp.bfloat16)
    ranks = jnp.dot(earlier, member.astype(jnp.bfloat16), preferred_element_type=jnp.float32)
    keys = jnp.where(member > 0.5, ranks, -1.0)
    key_col[...] = keys
    key_row[...] = keys.T

    for copy in halos:
        copy.wait_recv()
    row_at = lax.broadcasted_iota(jnp.int32, (row_count, 1), 0)
    own_docs = docs_ref[:, 0:1]
    halo_ids = jnp.where(me > 0, halo_docs[...], -1.0)[:, 0:1]
    docs_one = jnp.where(row_at == 0, halo_ids[7:8], pltpu.roll(docs_ref[...], 1, 0)[:, 0:1])
    docs_two = jnp.where(
        row_at == 0,
        halo_ids[6:7],
        jnp.where(row_at == 1, halo_ids[7:8], pltpu.roll(docs_ref[...], 2, 0)[:, 0:1]),
    )
    same_one, same_two = docs_one == own_docs, docs_two == own_docs

    def conv_tile(j, carry):
        at = pl.ds(pl.multiple_of(j * 128, 128), 128)
        products = inner_ref[:, at].astype(jnp.float32) * conv_ref[:, at].astype(jnp.float32)
        before = halo_inner[:, at].astype(jnp.float32) * halo_conv[:, at].astype(jnp.float32)
        one = jnp.where(row_at == 0, before[15:16], pltpu.roll(products, 1, 0))
        two = jnp.where(
            row_at == 0,
            before[14:15],
            jnp.where(row_at == 1, before[15:16], pltpu.roll(products, 2, 0)),
        )
        taps = taps_ref[:, at].astype(jnp.float32)
        conv = taps[2:3] * products
        conv = conv + jnp.where(same_one, taps[1:2] * one, 0.0)
        conv = conv + jnp.where(same_two, taps[0:1] * two, 0.0)
        value = (outer_ref[:, at].astype(jnp.float32) * conv).astype(jnp.bfloat16)
        branch[:, pl.ds(pl.multiple_of(t * wide + j * 128, 128), 128)] = value
        return carry

    lax.fori_loop(0, wide // 128, conv_tile, 0)

    def branch_region(index):
        return branch.at[:, column(index, wide)]

    region = branch_region(t)
    for d in range(1, chips):
        copy = remote(region, region, by_send.at[d], by_recv.at[d], (me, chip_at(d)))
        copy.start()
        sends.append(copy)
    copy = remote(region, region, bp_send.at[0], bp_recv.at[0], (me, partner))
    copy.start()
    sends.append(copy)
    weight_copies[3].wait()

    def project(index, first=False):
        step = min(256, cols)

        def tile(j, carry):
            at = pl.ds(pl.multiple_of(j * step, 128), step)
            rows = pl.ds(pl.multiple_of(index * wide, 128), wide)
            value = jnp.dot(
                branch[:, column(index, wide)], proj_w[rows, at], preferred_element_type=jnp.float32
            )
            acc[:, at] = value if first else acc[:, at] + value
            return carry

        lax.fori_loop(0, cols // step, tile, 0)

    project(t, True)
    other = branch_region(partner)
    remote(other, other, bp_send.at[0], bp_recv.at[0], (me, partner)).wait_recv()
    project(partner)
    for d in range(1, chips):
        source = chip_at(-d)
        region = branch_region(source)
        remote(region, region, by_send.at[d], by_recv.at[d], (me, partner)).wait_recv()
        copy = remote(region, region, bp_send.at[d], bp_recv.at[d], (me, partner))
        copy.start()
        sends.append(copy)
        project(source)
    for d in range(1, chips):
        source = chip_at(-d) + partner - t
        region = branch_region(source)
        remote(region, region, bp_send.at[d], bp_recv.at[d], (me, partner)).wait_recv()
        project(source)

    def resid_tile(j, total):
        at = pl.ds(pl.multiple_of(j * 128, 128), 128)
        value = (residual_ref[:, at].astype(jnp.float32) + acc[:, at]).astype(jnp.bfloat16)
        resid[:, at] = value
        value = value.astype(jnp.float32)
        return total + value * value

    total = lax.fori_loop(
        0, cols // 128, resid_tile, jnp.zeros((row_count, 128), jnp.float32)
    )
    squares[t] = jnp.broadcast_to(
        jnp.sum(total.T, axis=0, keepdims=True), (8, row_count)
    )
    for d in range(1, tp):
        copy = remote(
            squares.at[t], squares.at[t], s_send.at[d], s_recv.at[d], (me, lax.rem(t + d, tp))
        )
        copy.start()
        sends.append(copy)
    for d in range(1, tp):
        source = lax.rem(t + tp - d, tp)
        remote(
            squares.at[source], squares.at[source], s_send.at[d], s_recv.at[d], (me, source)
        ).wait_recv()
    total_sq = jnp.sum(squares[...], axis=0)[0:1]
    scale_row = lax.rsqrt(total_sq / (tp * cols) + EPS)
    scale = jnp.broadcast_to(scale_row, (128, row_count)).T

    def norm_tile(j, carry):
        at = pl.ds(pl.multiple_of(j * 128, 128), 128)
        value = resid[:, at].astype(jnp.float32) * scale * gain_ref[:, at].astype(jnp.float32)
        normed[:, at] = value.astype(jnp.bfloat16)
        return carry

    lax.fori_loop(0, cols // 128, norm_tile, 0)

    slot_rows = lax.broadcasted_iota(jnp.int32, (cap, row_count), 0).astype(jnp.float32)

    def choose(expert):
        select = jnp.where(slot_rows == key_row[pl.ds(expert, 1), :], 1.0, 0.0)
        out_ref[expert] = jnp.dot(
            select.astype(jnp.bfloat16), normed[...], preferred_element_type=jnp.float32
        ).astype(jnp.bfloat16)

    for k in range(1, n):
        there = lax.rem(me + k, n)
        choose(there)
        copy = remote(
            out_ref.at[there],
            piece.at[k, :, column(t, cols)],
            a_send.at[k],
            a_recv.at[k],
            (there, t),
        )
        copy.start()
        sends.append(copy)
        arrivals.append(copy)
    choose(me)
    own_in = pltpu.make_async_copy(out_ref.at[me], piece.at[0, :, column(t, cols)], own_sem.at[0])
    own_in.start()

    def fan_region(f, index):
        return piece.at[pl.ds(f * fan_blocks, fan_blocks), :, column(index, cols)]

    def fan_out(f):
        for k in range(f * fan_blocks, (f + 1) * fan_blocks):
            if k == 0:
                own_in.wait()
            else:
                arrivals[k - 1].wait_recv()
        region = fan_region(f, t)
        for d in range(1, chips):
            copy = remote(
                region, region, y_send.at[d, f], y_recv.at[d, f], (me, chip_at(d))
            )
            copy.start()
            sends.append(copy)
        copy = remote(region, region, p_send.at[0, f], p_recv.at[0, f], (me, partner))
        copy.start()
        sends.append(copy)

    def relay(f):
        for d in range(1, chips):
            source = chip_at(-d)
            region = fan_region(f, source)
            remote(
                region, region, y_send.at[d, f], y_recv.at[d, f], (me, partner)
            ).wait_recv()
            copy = remote(region, region, p_send.at[d, f], p_recv.at[d, f], (me, partner))
            copy.start()
            sends.append(copy)

    def hid_region(g, index):
        return hid.at[g, :, column(index, ffn_local)]

    def up_stage(g):
        for f in range(g * group_fans, (g + 1) * group_fans):
            for d in range(chips):
                region = fan_region(f, chip_at(-d) + partner - t)
                remote(
                    region, region, p_send.at[d, f], p_recv.at[d, f], (me, partner)
                ).wait_recv()
        if g == 0:
            weight_copies[0].wait()
            weight_copies[1].wait()
        step = min(256, ffn_local)

        def tile(j, carry):
            rows = piece[pl.ds(g * group_blocks, group_blocks)].reshape(group_rows, tp * cols)
            at = pl.ds(pl.multiple_of(j * step, 128), step)
            gate_val = jnp.dot(rows, gate_w[:, at], preferred_element_type=jnp.float32)
            up_val = jnp.dot(rows, up_w[:, at], preferred_element_type=jnp.float32)
            hidden = (jax.nn.silu(gate_val) * up_val).astype(jnp.bfloat16)
            hid[g, :, pl.ds(pl.multiple_of(t * ffn_local + j * step, 128), step)] = hidden
            return carry

        lax.fori_loop(0, ffn_local // step, tile, 0)
        region = hid_region(g, t)
        for d in range(1, chips):
            copy = remote(
                region, region, hy_send.at[d, g], hy_recv.at[d, g], (me, chip_at(d))
            )
            copy.start()
            sends.append(copy)
        copy = remote(region, region, hp_send.at[0, g], hp_recv.at[0, g], (me, partner))
        copy.start()
        sends.append(copy)

    def relay_hidden(g):
        for d in range(1, chips):
            region = hid_region(g, chip_at(-d))
            remote(
                region, region, hy_send.at[d, g], hy_recv.at[d, g], (me, partner)
            ).wait_recv()
            copy = remote(region, region, hp_send.at[d, g], hp_recv.at[d, g], (me, partner))
            copy.start()
            sends.append(copy)

    returns = []

    def down_stage(g):
        for d in range(chips):
            region = hid_region(g, chip_at(-d) + partner - t)
            remote(
                region, region, hp_send.at[d, g], hp_recv.at[d, g], (me, partner)
            ).wait_recv()
        if g == 0:
            weight_copies[2].wait()
        step = min(256, cols)

        def tile(j, carry):
            at = pl.ds(pl.multiple_of(j * step, 128), step)
            value = jnp.dot(hid[g], down_w[:, at], preferred_element_type=jnp.float32)
            eo[pl.ds(g * group_blocks, group_blocks), :, at] = value.astype(
                jnp.bfloat16
            ).reshape(group_blocks, cap, step)
            return carry

        lax.fori_loop(0, cols // step, tile, 0)
        for k in range(g * group_blocks, (g + 1) * group_blocks):
            if k == 0:
                copy = pltpu.make_async_copy(eo.at[0], ret_ref.at[me], own_sem.at[1])
            else:
                copy = remote(
                    eo.at[k],
                    ret_ref.at[me],
                    r_send.at[k],
                    r_recv.at[k],
                    (lax.rem(me + n - k, n), t),
                )
            copy.start()
            returns.append(copy)

    def fans_of(g):
        return range(g * group_fans, (g + 1) * group_fans)

    ahead = min(2, groups)
    for g in range(ahead):
        for f in fans_of(g):
            fan_out(f)
    for g in range(groups):
        for f in fans_of(g):
            relay(f)
        up_stage(g)
        if g + ahead < groups:
            for f in fans_of(g + ahead):
                fan_out(f)
        if g >= 1:
            relay_hidden(g - 1)
            down_stage(g - 1)
    relay_hidden(groups - 1)
    down_stage(groups - 1)

    slot_lanes = lax.broadcasted_iota(jnp.int32, (row_count, cap), 1).astype(jnp.float32)
    for g in range(groups):
        members = range(g * group_blocks, (g + 1) * group_blocks)
        for k in members:
            if k == 0:
                returns[0].wait()
            else:
                there = lax.rem(me + k, n)
                returns[k].wait_send()
                remote(
                    eo.at[k], ret_ref.at[there], r_send.at[k], r_recv.at[k], (there, t)
                ).wait_recv()
        chosen = []
        for k in members:
            there = lax.rem(me + k, n)
            here = lanes == there
            key = jnp.sum(jnp.where(here, key_col[...], 0.0), axis=1, keepdims=True)
            weight = jnp.sum(jnp.where(here, mix_col[...], 0.0), axis=1, keepdims=True)
            select = jnp.where(slot_lanes == key, 1.0, 0.0).astype(jnp.bfloat16)
            chosen.append((there, select, weight))
        step = min(256, cols)

        def combine(j, carry):
            at = pl.ds(pl.multiple_of(j * step, 128), step)
            value = jnp.zeros((row_count, step), jnp.float32) if g == 0 else acc[:, at]
            for there, select, weight in chosen:
                value = value + weight * jnp.dot(
                    select, ret_ref[there, :, at], preferred_element_type=jnp.float32
                )
            if g == groups - 1:
                result_ref[:, at] = (resid[:, at].astype(jnp.float32) + value).astype(jnp.bfloat16)
            else:
                acc[:, at] = value
            return carry

        lax.fori_loop(0, cols // step, combine, 0)
    for copy in sends:
        copy.wait_send()


def whole_layer(blocks, weights):
    n, tp = lax.axis_size("sp"), lax.axis_size("tp")
    row_count, wide = blocks[0].shape
    cols = blocks[5].shape[1]
    cap = 4 * row_count // n
    chips = tp // 2
    rows = n * cap
    groups = max(1, min(4, rows // 256))
    fans = min(n, 2 * groups)
    projection, gate_weight, _, down_weight = weights
    width, ffn_local = gate_weight.shape[1], gate_weight.shape[2]
    ffn = down_weight.shape[1]
    dma = pltpu.SemaphoreType.DMA
    bf16, f32 = jnp.bfloat16, jnp.float32
    flops = 2 * rows * width * ffn_local * 2 + 2 * rows * ffn * cols
    return pl.pallas_call(
        functools.partial(expert_kernel, n, tp),
        out_shape=jax.ShapeDtypeStruct((row_count, cols), bf16),
        in_specs=[pl.BlockSpec(memory_space=pltpu.VMEM)] * len(blocks)
        + [pl.BlockSpec(memory_space=pl.ANY)] * len(weights),
        out_specs=pl.BlockSpec(memory_space=pltpu.VMEM),
        scratch_shapes=[
            pltpu.VMEM((n, cap, cols), bf16),
            pltpu.VMEM((n, cap, cols), bf16),
            pltpu.VMEM((row_count, wide * tp), bf16),
            pltpu.VMEM(projection.shape, bf16),
            pltpu.VMEM((row_count, cols), f32),
            pltpu.VMEM((row_count, cols), bf16),
            pltpu.VMEM((row_count, cols), bf16),
            pltpu.VMEM((tp, 8, row_count), f32),
            pltpu.VMEM((row_count, 128), f32),
            pltpu.VMEM((128, row_count), f32),
            pltpu.VMEM((row_count, 128), f32),
            pltpu.VMEM((16, wide), bf16),
            pltpu.VMEM((16, wide), bf16),
            pltpu.VMEM((8, 128), f32),
            pltpu.VMEM((n, cap, width), bf16),
            pltpu.VMEM((groups, rows // groups, ffn), bf16),
            pltpu.VMEM((n, cap, cols), bf16),
            pltpu.VMEM((width, ffn_local), bf16),
            pltpu.VMEM((width, ffn_local), bf16),
            pltpu.VMEM((ffn, cols), bf16),
            dma((4,)),
            dma((2,)),
            dma((n,)),
            dma((n,)),
            dma((chips, fans)),
            dma((chips, fans)),
            dma((chips, fans)),
            dma((chips, fans)),
            dma((chips, groups)),
            dma((chips, groups)),
            dma((chips, groups)),
            dma((chips, groups)),
            dma((n,)),
            dma((n,)),
            dma((3,)),
            dma((3,)),
            dma((chips,)),
            dma((chips,)),
            dma((chips,)),
            dma((chips,)),
            dma((tp,)),
            dma((tp,)),
        ],
        compiler_params=pltpu.CompilerParams(
            collective_id=0, has_side_effects=True, vmem_limit_bytes=56 * 1024 * 1024
        ),
        cost_estimate=pl.CostEstimate(
            flops=flops, bytes_accessed=3 * width * ffn_local * 2, transcendentals=0
        ),
        name="layer",
    )(*blocks, *weights)


def per_device(
    outer_gate,
    inner_gate,
    conv_input,
    conv_weight,
    doc_ids,
    output_weight,
    residual,
    norm_gain,
    expert_ids,
    group_weight,
    expert_weight,
    gate_weight,
    up_weight,
    down_weight,
):
    row_count = conv_input.shape[0]
    docs = jnp.broadcast_to(doc_ids.astype(jnp.float32)[:, None], (row_count, 128))
    mix_weight = (
        group_weight[:, None] * expert_weight / jnp.sum(expert_weight, axis=1, keepdims=True)
    )
    return whole_layer(
        (
            outer_gate,
            inner_gate,
            conv_input,
            conv_weight,
            docs,
            residual,
            norm_gain[None, :],
            expert_ids,
            mix_weight,
        ),
        (output_weight, gate_weight, up_weight, down_weight),
    )


def solution(mesh):
    return jax.shard_map(
        per_device,
        mesh=mesh,
        in_specs=(
            P("sp", "tp"),
            P("sp", "tp"),
            P("sp", "tp"),
            P(None, "tp"),
            P("sp"),
            P(None, "tp"),
            P("sp", "tp"),
            P("tp"),
            P("sp", None),
            P("sp"),
            P("sp", None),
            P("sp", None, "tp"),
            P("sp", None, "tp"),
            P("sp", None, "tp"),
        ),
        out_specs=P("sp", "tp"),
        check_vma=False,
    )
```

```python
import functools

import jax
import jax.numpy as jnp
from jax import lax
from jax.experimental import pallas as pl
from jax.experimental.pallas import tpu as pltpu
from jax.sharding import PartitionSpec as P

EPS = 1e-06
MESH = pl.DeviceIdType.MESH


def remote(src, dst, send_sem, recv_sem, device):
    return pltpu.make_async_remote_copy(
        src_ref=src,
        dst_ref=dst,
        send_sem=send_sem,
        recv_sem=recv_sem,
        device_id=device,
        device_id_type=MESH,
    )


def expert_kernel(
    n,
    tp,
    outer_ref,
    inner_ref,
    conv_ref,
    taps_ref,
    docs_ref,
    residual_ref,
    gain_ref,
    ids_ref,
    mix_ref,
    proj_hbm,
    gate_hbm,
    up_hbm,
    down_hbm,
    result_ref,
    out_ref,
    ret_ref,
    branch,
    proj_w,
    acc,
    resid,
    normed,
    squares,
    key_col,
    key_row,
    mix_col,
    halo_inner,
    halo_conv,
    halo_docs,
    piece,
    hid,
    eo,
    gate_w,
    up_w,
    down_w,
    w_sem,
    own_sem,
    a_send,
    a_recv,
    y_send,
    y_recv,
    p_send,
    p_recv,
    hy_send,
    hy_recv,
    hp_send,
    hp_recv,
    r_send,
    r_recv,
    h_send,
    h_recv,
    by_send,
    by_recv,
    bp_send,
    bp_recv,
    s_send,
    s_recv,
):
    me = lax.axis_index("sp")
    t = lax.axis_index("tp")
    later = [k for k in range(1, n) if k != 2]
    order = [0, 2] + sorted(later, key=lambda k: -min(k, n - k))
    chips = tp // 2
    y, core = lax.div(t, 2), lax.rem(t, 2)
    partner = t + 1 - 2 * core
    cap, cols = out_ref.shape[1], out_ref.shape[2]
    ffn_local = gate_w.shape[1]
    groups, group_rows = hid.shape[0], hid.shape[1]
    fans = p_send.shape[1]
    fan_blocks = n // fans
    group_fans = fans // groups
    group_blocks = n // groups

    def column(index, width):
        return pl.ds(pl.multiple_of(index * width, 128), width)

    def chip_at(delta):
        return lax.rem(y + delta + chips, chips) * 2 + core

    weight_copies = [
        pltpu.make_async_copy(source, target, w_sem.at[i])
        for i, (source, target) in enumerate(
            (
                (gate_hbm.at[0], gate_w),
                (up_hbm.at[0], up_w),
                (down_hbm.at[0], down_w),
                (proj_hbm, proj_w),
            )
        )
    ]
    for i in (3, 0, 1, 2):
        weight_copies[i].start()

    barrier = pltpu.get_barrier_semaphore()
    for k in range(1, n):
        pl.semaphore_signal(
            barrier, inc=1, device_id=(lax.rem(me + k, n), t), device_id_type=MESH
        )
    for d in range(1, tp):
        pl.semaphore_signal(
            barrier, inc=1, device_id=(me, lax.rem(t + d, tp)), device_id_type=MESH
        )
    pl.semaphore_wait(barrier, n - 1 + tp - 1)

    sends = []
    arrivals = []
    row_count = residual_ref.shape[0]
    wide = branch.shape[1] // tp

    halos = []
    following = (lax.rem(me + 1, n), t)
    for i, (source, target) in enumerate(
        (
            (inner_ref.at[pl.ds(row_count - 16, 16)], halo_inner),
            (conv_ref.at[pl.ds(row_count - 16, 16)], halo_conv),
            (docs_ref.at[pl.ds(row_count - 8, 8)], halo_docs),
        )
    ):
        copy = remote(source, target, h_send.at[i], h_recv.at[i], following)
        copy.start()
        halos.append(copy)
        sends.append(copy)

    lanes = lax.broadcasted_iota(jnp.int32, (row_count, 128), 1)
    first_id, second_id = ids_ref[:, 0:1], ids_ref[:, 1:2]
    is_first, is_second = lanes == first_id, lanes == second_id
    mix_col[...] = jnp.where(is_first, mix_ref[:, 0:1], 0.0) + jnp.where(
        is_second, mix_ref[:, 1:2], 0.0
    )
    member = jnp.where(is_first, 1.0, 0.0) + jnp.where(is_second, 1.0, 0.0)
    earlier = jnp.where(
        lax.broadcasted_iota(jnp.int32, (row_count, row_count), 1)
        < lax.broadcasted_iota(jnp.int32, (row_count, row_count), 0),
        1.0,
        0.0,
    ).astype(jnp.bfloat16)
    ranks = jnp.dot(earlier, member.astype(jnp.bfloat16), preferred_element_type=jnp.float32)
    keys = jnp.where(member > 0.5, ranks, -1.0)
    key_col[...] = keys
    key_row[...] = keys.T

    for copy in halos:
        copy.wait_recv()
    row_at = lax.broadcasted_iota(jnp.int32, (row_count, 1), 0)
    own_docs = docs_ref[:, 0:1]
    halo_ids = jnp.where(me > 0, halo_docs[...], -1.0)[:, 0:1]
    docs_one = jnp.where(row_at == 0, halo_ids[7:8], pltpu.roll(docs_ref[...], 1, 0)[:, 0:1])
    docs_two = jnp.where(
        row_at == 0,
        halo_ids[6:7],
        jnp.where(row_at == 1, halo_ids[7:8], pltpu.roll(docs_ref[...], 2, 0)[:, 0:1]),
    )
    same_one, same_two = docs_one == own_docs, docs_two == own_docs

    def conv_tile(j, carry):
        at = pl.ds(pl.multiple_of(j * 128, 128), 128)
        products = inner_ref[:, at].astype(jnp.float32) * conv_ref[:, at].astype(jnp.float32)
        before = halo_inner[:, at].astype(jnp.float32) * halo_conv[:, at].astype(jnp.float32)
        one = jnp.where(row_at == 0, before[15:16], pltpu.roll(products, 1, 0))
        two = jnp.where(
            row_at == 0,
            before[14:15],
            jnp.where(row_at == 1, before[15:16], pltpu.roll(products, 2, 0)),
        )
        taps = taps_ref[:, at].astype(jnp.float32)
        conv = taps[2:3] * products
        conv = conv + jnp.where(same_one, taps[1:2] * one, 0.0)
        conv = conv + jnp.where(same_two, taps[0:1] * two, 0.0)
        value = (outer_ref[:, at].astype(jnp.float32) * conv).astype(jnp.bfloat16)
        branch[:, pl.ds(pl.multiple_of(t * wide + j * 128, 128), 128)] = value
        return carry

    lax.fori_loop(0, wide // 128, conv_tile, 0)

    def branch_region(index):
        return branch.at[:, column(index, wide)]

    region = branch_region(t)
    for d in range(1, chips):
        copy = remote(region, region, by_send.at[d], by_recv.at[d], (me, chip_at(d)))
        copy.start()
        sends.append(copy)
    copy = remote(region, region, bp_send.at[0], bp_recv.at[0], (me, partner))
    copy.start()
    sends.append(copy)
    weight_copies[3].wait()

    def project(index, first=False):
        step = min(256, cols)

        def tile(j, carry):
            at = pl.ds(pl.multiple_of(j * step, 128), step)
            rows = pl.ds(pl.multiple_of(index * wide, 128), wide)
            value = jnp.dot(
                branch[:, column(index, wide)], proj_w[rows, at], preferred_element_type=jnp.float32
            )
            acc[:, at] = value if first else acc[:, at] + value
            return carry

        lax.fori_loop(0, cols // step, tile, 0)

    project(t, True)
    other = branch_region(partner)
    remote(other, other, bp_send.at[0], bp_recv.at[0], (me, partner)).wait_recv()
    project(partner)
    for d in range(1, chips):
        source = chip_at(-d)
        region = branch_region(source)
        remote(region, region, by_send.at[d], by_recv.at[d], (me, partner)).wait_recv()
        copy = remote(region, region, bp_send.at[d], bp_recv.at[d], (me, partner))
        copy.start()
        sends.append(copy)
        project(source)
    for d in range(1, chips):
        source = chip_at(-d) + partner - t
        region = branch_region(source)
        remote(region, region, bp_send.at[d], bp_recv.at[d], (me, partner)).wait_recv()
        project(source)

    def resid_tile(j, total):
        at = pl.ds(pl.multiple_of(j * 128, 128), 128)
        value = (residual_ref[:, at].astype(jnp.float32) + acc[:, at]).astype(jnp.bfloat16)
        resid[:, at] = value
        value = value.astype(jnp.float32)
        return total + value * value

    total = lax.fori_loop(
        0, cols // 128, resid_tile, jnp.zeros((row_count, 128), jnp.float32)
    )
    squares[t] = jnp.broadcast_to(
        jnp.sum(total.T, axis=0, keepdims=True), (8, row_count)
    )
    for d in range(1, tp):
        copy = remote(
            squares.at[t], squares.at[t], s_send.at[d], s_recv.at[d], (me, lax.rem(t + d, tp))
        )
        copy.start()
        sends.append(copy)
    for d in range(1, tp):
        source = lax.rem(t + tp - d, tp)
        remote(
            squares.at[source], squares.at[source], s_send.at[d], s_recv.at[d], (me, source)
        ).wait_recv()
    total_sq = jnp.sum(squares[...], axis=0)[0:1]
    scale_row = lax.rsqrt(total_sq / (tp * cols) + EPS)
    scale = jnp.broadcast_to(scale_row, (128, row_count)).T

    def norm_tile(j, carry):
        at = pl.ds(pl.multiple_of(j * 128, 128), 128)
        value = resid[:, at].astype(jnp.float32) * scale * gain_ref[:, at].astype(jnp.float32)
        normed[:, at] = value.astype(jnp.bfloat16)
        return carry

    lax.fori_loop(0, cols // 128, norm_tile, 0)

    slot_rows = lax.broadcasted_iota(jnp.int32, (cap, row_count), 0).astype(jnp.float32)

    def choose(expert):
        select = jnp.where(slot_rows == key_row[pl.ds(expert, 1), :], 1.0, 0.0)
        out_ref[expert] = jnp.dot(
            select.astype(jnp.bfloat16), normed[...], preferred_element_type=jnp.float32
        ).astype(jnp.bfloat16)

    for k in range(1, n):
        there = lax.rem(me + order[k], n)
        choose(there)
        copy = remote(
            out_ref.at[there],
            piece.at[k, :, column(t, cols)],
            a_send.at[k],
            a_recv.at[k],
            (there, t),
        )
        copy.start()
        sends.append(copy)
        arrivals.append(copy)
    choose(me)
    own_in = pltpu.make_async_copy(out_ref.at[me], piece.at[0, :, column(t, cols)], own_sem.at[0])
    own_in.start()

    def fan_region(f, index):
        return piece.at[pl.ds(f * fan_blocks, fan_blocks), :, column(index, cols)]

    def fan_out(f):
        for k in range(f * fan_blocks, (f + 1) * fan_blocks):
            if k == 0:
                own_in.wait()
            else:
                arrivals[k - 1].wait_recv()
        region = fan_region(f, t)
        for d in range(1, chips):
            copy = remote(
                region, region, y_send.at[d, f], y_recv.at[d, f], (me, chip_at(d))
            )
            copy.start()
            sends.append(copy)
        copy = remote(region, region, p_send.at[0, f], p_recv.at[0, f], (me, partner))
        copy.start()
        sends.append(copy)

    def relay(f):
        for d in range(1, chips):
            source = chip_at(-d)
            region = fan_region(f, source)
            remote(
                region, region, y_send.at[d, f], y_recv.at[d, f], (me, partner)
            ).wait_recv()
            copy = remote(region, region, p_send.at[d, f], p_recv.at[d, f], (me, partner))
            copy.start()
            sends.append(copy)

    def hid_region(g, index):
        return hid.at[g, :, column(index, ffn_local)]

    def up_stage(g):
        for f in range(g * group_fans, (g + 1) * group_fans):
            for d in range(chips):
                region = fan_region(f, chip_at(-d) + partner - t)
                remote(
                    region, region, p_send.at[d, f], p_recv.at[d, f], (me, partner)
                ).wait_recv()
        if g == 0:
            weight_copies[0].wait()
            weight_copies[1].wait()
        step = min(256, ffn_local)

        def tile(j, carry):
            rows = piece[pl.ds(g * group_blocks, group_blocks)].reshape(group_rows, tp * cols)
            at = pl.ds(pl.multiple_of(j * step, 128), step)
            gate_val = jnp.dot(rows, gate_w[:, at], preferred_element_type=jnp.float32)
            up_val = jnp.dot(rows, up_w[:, at], preferred_element_type=jnp.float32)
            hidden = (jax.nn.silu(gate_val) * up_val).astype(jnp.bfloat16)
            hid[g, :, pl.ds(pl.multiple_of(t * ffn_local + j * step, 128), step)] = hidden
            return carry

        lax.fori_loop(0, ffn_local // step, tile, 0)
        region = hid_region(g, t)
        for d in range(1, chips):
            copy = remote(
                region, region, hy_send.at[d, g], hy_recv.at[d, g], (me, chip_at(d))
            )
            copy.start()
            sends.append(copy)
        copy = remote(region, region, hp_send.at[0, g], hp_recv.at[0, g], (me, partner))
        copy.start()
        sends.append(copy)

    def relay_hidden(g):
        for d in range(1, chips):
            region = hid_region(g, chip_at(-d))
            remote(
                region, region, hy_send.at[d, g], hy_recv.at[d, g], (me, partner)
            ).wait_recv()
            copy = remote(region, region, hp_send.at[d, g], hp_recv.at[d, g], (me, partner))
            copy.start()
            sends.append(copy)

    returns = []

    def down_stage(g):
        for d in range(chips):
            region = hid_region(g, chip_at(-d) + partner - t)
            remote(
                region, region, hp_send.at[d, g], hp_recv.at[d, g], (me, partner)
            ).wait_recv()
        if g == 0:
            weight_copies[2].wait()
        step = min(256, cols)

        def tile(j, carry):
            at = pl.ds(pl.multiple_of(j * step, 128), step)
            value = jnp.dot(hid[g], down_w[:, at], preferred_element_type=jnp.float32)
            eo[pl.ds(g * group_blocks, group_blocks), :, at] = value.astype(
                jnp.bfloat16
            ).reshape(group_blocks, cap, step)
            return carry

        lax.fori_loop(0, cols // step, tile, 0)
        for k in range(g * group_blocks, (g + 1) * group_blocks):
            if k == 0:
                copy = pltpu.make_async_copy(eo.at[0], ret_ref.at[me], own_sem.at[1])
            else:
                copy = remote(
                    eo.at[k],
                    ret_ref.at[me],
                    r_send.at[k],
                    r_recv.at[k],
                    (lax.rem(me + n - order[k], n), t),
                )
            copy.start()
            returns.append(copy)

    def fans_of(g):
        return range(g * group_fans, (g + 1) * group_fans)

    ahead = min(2, groups)
    for g in range(ahead):
        for f in fans_of(g):
            fan_out(f)
    for g in range(groups):
        for f in fans_of(g):
            relay(f)
        up_stage(g)
        if g + ahead < groups:
            for f in fans_of(g + ahead):
                fan_out(f)
        if g >= 1:
            relay_hidden(g - 1)
            down_stage(g - 1)
    relay_hidden(groups - 1)
    down_stage(groups - 1)

    slot_lanes = lax.broadcasted_iota(jnp.int32, (row_count, cap), 1).astype(jnp.float32)
    for g in range(groups):
        members = range(g * group_blocks, (g + 1) * group_blocks)
        for k in members:
            if k == 0:
                returns[0].wait()
            else:
                there = lax.rem(me + order[k], n)
                returns[k].wait_send()
                remote(
                    eo.at[k], ret_ref.at[there], r_send.at[k], r_recv.at[k], (there, t)
                ).wait_recv()
        chosen = []
        for k in members:
            there = lax.rem(me + order[k], n)
            here = lanes == there
            key = jnp.sum(jnp.where(here, key_col[...], 0.0), axis=1, keepdims=True)
            weight = jnp.sum(jnp.where(here, mix_col[...], 0.0), axis=1, keepdims=True)
            select = jnp.where(slot_lanes == key, 1.0, 0.0).astype(jnp.bfloat16)
            chosen.append((there, select, weight))
        step = min(256, cols)

        def combine(j, carry):
            at = pl.ds(pl.multiple_of(j * step, 128), step)
            value = jnp.zeros((row_count, step), jnp.float32) if g == 0 else acc[:, at]
            for there, select, weight in chosen:
                value = value + weight * jnp.dot(
                    select, ret_ref[there, :, at], preferred_element_type=jnp.float32
                )
            if g == groups - 1:
                result_ref[:, at] = (resid[:, at].astype(jnp.float32) + value).astype(jnp.bfloat16)
            else:
                acc[:, at] = value
            return carry

        lax.fori_loop(0, cols // step, combine, 0)
    for copy in sends:
        copy.wait_send()


def whole_layer(blocks, weights):
    n, tp = lax.axis_size("sp"), lax.axis_size("tp")
    row_count, wide = blocks[0].shape
    cols = blocks[5].shape[1]
    cap = 4 * row_count // n
    chips = tp // 2
    rows = n * cap
    groups = max(1, min(4, rows // 256))
    fans = min(n, 2 * groups)
    projection, gate_weight, _, down_weight = weights
    width, ffn_local = gate_weight.shape[1], gate_weight.shape[2]
    ffn = down_weight.shape[1]
    dma = pltpu.SemaphoreType.DMA
    bf16, f32 = jnp.bfloat16, jnp.float32
    flops = 2 * rows * width * ffn_local * 2 + 2 * rows * ffn * cols
    return pl.pallas_call(
        functools.partial(expert_kernel, n, tp),
        out_shape=jax.ShapeDtypeStruct((row_count, cols), bf16),
        in_specs=[pl.BlockSpec(memory_space=pltpu.VMEM)] * len(blocks)
        + [pl.BlockSpec(memory_space=pl.ANY)] * len(weights),
        out_specs=pl.BlockSpec(memory_space=pltpu.VMEM),
        scratch_shapes=[
            pltpu.VMEM((n, cap, cols), bf16),
            pltpu.VMEM((n, cap, cols), bf16),
            pltpu.VMEM((row_count, wide * tp), bf16),
            pltpu.VMEM(projection.shape, bf16),
            pltpu.VMEM((row_count, cols), f32),
            pltpu.VMEM((row_count, cols), bf16),
            pltpu.VMEM((row_count, cols), bf16),
            pltpu.VMEM((tp, 8, row_count), f32),
            pltpu.VMEM((row_count, 128), f32),
            pltpu.VMEM((128, row_count), f32),
            pltpu.VMEM((row_count, 128), f32),
            pltpu.VMEM((16, wide), bf16),
            pltpu.VMEM((16, wide), bf16),
            pltpu.VMEM((8, 128), f32),
            pltpu.VMEM((n, cap, width), bf16),
            pltpu.VMEM((groups, rows // groups, ffn), bf16),
            pltpu.VMEM((n, cap, cols), bf16),
            pltpu.VMEM((width, ffn_local), bf16),
            pltpu.VMEM((width, ffn_local), bf16),
            pltpu.VMEM((ffn, cols), bf16),
            dma((4,)),
            dma((2,)),
            dma((n,)),
            dma((n,)),
            dma((chips, fans)),
            dma((chips, fans)),
            dma((chips, fans)),
            dma((chips, fans)),
            dma((chips, groups)),
            dma((chips, groups)),
            dma((chips, groups)),
            dma((chips, groups)),
            dma((n,)),
            dma((n,)),
            dma((3,)),
            dma((3,)),
            dma((chips,)),
            dma((chips,)),
            dma((chips,)),
            dma((chips,)),
            dma((tp,)),
            dma((tp,)),
        ],
        compiler_params=pltpu.CompilerParams(
            collective_id=0, has_side_effects=True, vmem_limit_bytes=56 * 1024 * 1024
        ),
        cost_estimate=pl.CostEstimate(
            flops=flops, bytes_accessed=3 * width * ffn_local * 2, transcendentals=0
        ),
        name="layer",
    )(*blocks, *weights)


def per_device(
    outer_gate,
    inner_gate,
    conv_input,
    conv_weight,
    doc_ids,
    output_weight,
    residual,
    norm_gain,
    expert_ids,
    group_weight,
    expert_weight,
    gate_weight,
    up_weight,
    down_weight,
):
    row_count = conv_input.shape[0]
    docs = jnp.broadcast_to(doc_ids.astype(jnp.float32)[:, None], (row_count, 128))
    mix_weight = (
        group_weight[:, None] * expert_weight / jnp.sum(expert_weight, axis=1, keepdims=True)
    )
    return whole_layer(
        (
            outer_gate,
            inner_gate,
            conv_input,
            conv_weight,
            docs,
            residual,
            norm_gain[None, :],
            expert_ids,
            mix_weight,
        ),
        (output_weight, gate_weight, up_weight, down_weight),
    )


def solution(mesh):
    return jax.shard_map(
        per_device,
        mesh=mesh,
        in_specs=(
            P("sp", "tp"),
            P("sp", "tp"),
            P("sp", "tp"),
            P(None, "tp"),
            P("sp"),
            P(None, "tp"),
            P("sp", "tp"),
            P("tp"),
            P("sp", None),
            P("sp"),
            P("sp", None),
            P("sp", None, "tp"),
            P("sp", None, "tp"),
            P("sp", None, "tp"),
        ),
        out_specs=P("sp", "tp"),
        check_vma=False,
    )
```
